32 devices in a mesh: sp: 8 (over z, y), dp: 4 (over x, core).
Axes of the slice: x: 2, y: 2, z: 4, core: 2. Of those that a mesh axis runs over, the one named last changes fastest.
Arguments:
- tokens: bfloat16 [4, 2560, 2048], P('dp', 'sp'), may hold values from -6 to 6
- w_query: bfloat16 [2048, 1024], P('dp', 'sp'), may hold values from -0.125 to 0.125
- w_key: bfloat16 [2048, 1024], P('dp', 'sp'), may hold values from -0.125 to 0.125
- w_value: bfloat16 [2048, 1024], P('dp', 'sp'), may hold values from -0.125 to 0.125
- w_output: bfloat16 [1024, 2048], P('sp', 'dp'), may hold values from -0.1875 to 0.1875
- qk_gain: float32 [2, 64], replicated, may hold values from 0.4 to 7
- decay_sums: float32 [4, 16, 2560], P('dp', 'sp'), may hold values from -512 to 0, as said below
Outputs:
- layer_out: bfloat16 [4, 2560, 2048], P('dp', 'sp')
The draws below stay inside these ranges and needn't reach their ends.
Inputs may be any that keep to these rules, and one draw needn't show every extreme that they name: `decay_sums`: each row is non-increasing along positions.
All inputs are finite; a program needn't handle non-finite values.
Results may differ from the reference program's by a relative error of at most 0.0075.
The reference program's roundings to bfloat16 on the way (of `query_proj`, `key_proj`, `value_proj`, `query_unit`, `key_unit`, `probs` and `head_out`) count: a program that leaves them out, or rounds other values in their place, can miss the bound.
Values may be sent and summed in bfloat16 or wider, within the bound.
A program may use at most 128 MiB of HBM per device.

```python
import jax
import jax.numpy as jnp
from jax import lax

D = 2048
HEADS = 16
HEAD_DIM = 64
TOK_DEV = 320
LENGTH = 2560
SEQS = 4


def draw_qk_gain(key, part):
    return jnp.clip(1.0 + 0.25 * jax.random.normal(key, (2, HEAD_DIM), jnp.float32), 0.4, 1.8)


def draw_decay_sums(key, part):
    streams = jax.random.split(key, 5)
    chance = 0.5
    quick = jax.random.bernoulli(streams[0], chance, (SEQS, HEADS, 1))
    quick_rate = 1.0 / jax.random.uniform(streams[1], (SEQS, HEADS, 1), jnp.float32, 30.0, 100.0)
    slow_rate = jax.random.uniform(streams[2], (SEQS, HEADS, 1), jnp.float32, 0.2, 0.8) / LENGTH
    rate = jnp.where(quick, quick_rate, slow_rate)
    spans = LENGTH // TOK_DEV
    factor = jnp.exp(jax.random.uniform(streams[3], (SEQS, HEADS, spans), jnp.float32, -1.05, 1.05))
    factor = jnp.repeat(factor, TOK_DEV, axis=2)
    rough = jax.random.uniform(streams[4], (SEQS, HEADS, LENGTH), jnp.float32, 0.2, 1.8)
    return -jnp.cumsum(rate * factor * rough, axis=2)


def steps_of(own_key, dims, shards, smallest, largest):
    level, own = 1.0, jax.random.fold_in(own_key, 6)
    for position, parts in shards:
        heights = jnp.exp(jax.random.uniform(jax.random.fold_in(own, position), (parts,), jnp.float32, smallest / len(shards), largest / len(shards)))
        level = level * jnp.repeat(heights, dims[position] // parts).reshape([-1 if axis == position else 1 for axis in range(len(dims))])
    return level


def normal_values(rng, extent, width, bound, pieces=(), held_as=jnp.bfloat16):
    level = steps_of(rng, extent, pieces, -0.22, 0.18) if pieces else 1.0
    drawn = jax.random.normal(rng, extent, jnp.float32) * width * level
    return jnp.minimum(jnp.maximum(drawn, -bound), bound).astype(held_as)


def setup_inputs(seed: int = 0) -> dict:
    key_of = jax.random.split(jax.random.key(seed), 8)
    return {
        "tokens": normal_values(key_of[0], (SEQS, LENGTH, D), 1.0, 6.0, ((0, 4), (1, 8))),
        "w_query": normal_values(key_of[1], (D, HEADS * HEAD_DIM), D ** -0.5, 0.125, ((0, 4), (1, 8))),
        "w_key": normal_values(key_of[2], (D, HEADS * HEAD_DIM), D ** -0.5, 0.125, ((0, 4), (1, 8))),
        "w_value": normal_values(key_of[3], (D, HEADS * HEAD_DIM), D ** -0.5, 0.125, ((0, 4), (1, 8))),
        "w_output": normal_values(key_of[4], (HEADS * HEAD_DIM, D), (HEADS * HEAD_DIM) ** -0.5, 0.1875, ((0, 8), (1, 4))),
        "qk_gain": draw_qk_gain(jax.random.fold_in(key_of[7], 71), 0),
        "decay_sums": draw_decay_sums(jax.random.fold_in(key_of[7], 71), 0),
    }


def normalize(values):
    values = values.astype(jnp.float32)
    return values * lax.rsqrt(lax.optimization_barrier(jnp.mean(values * values, axis=-1, keepdims=True)) + 1e-06)

def attend(query_unit, key_unit, value_rows, decay_rows):
    length = query_unit.shape[0]
    block = min(512, length)
    key_place = jnp.arange(length, dtype=jnp.int32)
    keys_wide = key_unit.astype(jnp.float32)
    values_wide = value_rows.astype(jnp.float32)

    def one_block(index):
        start = (index * block).astype(jnp.int32)
        query_block = lax.dynamic_slice_in_dim(query_unit, start, block, 0).astype(jnp.float32)
        decay_block = lax.dynamic_slice_in_dim(decay_rows, start, block, 1)
        scores = jnp.einsum('qhd,khd->hqk', query_block, keys_wide, precision=lax.Precision.HIGHEST)
        scores = scores + decay_block[:, :, None] - decay_rows[:, None, :]
        query_place = start + jnp.arange(block, dtype=jnp.int32)
        scores = jnp.where(key_place[None, None, :] <= query_place[None, :, None], scores, -jnp.inf)
        peak = lax.optimization_barrier(jnp.max(scores, axis=-1, keepdims=True))
        weights = jnp.exp(scores - peak)
        probs = (weights / lax.optimization_barrier(jnp.sum(weights, axis=-1, keepdims=True))).astype(jnp.bfloat16)
        return jnp.einsum('hqk,khd->qhd', probs.astype(jnp.float32), values_wide, precision=lax.Precision.HIGHEST)
    blocks = lax.map(one_block, jnp.arange(length // block, dtype=jnp.int32))
    return blocks.reshape(length, query_unit.shape[1], query_unit.shape[2])

def reference(tokens, w_query, w_key, w_value, w_output, qk_gain, decay_sums):

    def one_sequence(pair):
        own_rows, decay_rows = pair
        length = own_rows.shape[0]
        query_proj = jnp.dot(own_rows, w_query, preferred_element_type=jnp.float32).astype(jnp.bfloat16)
        key_proj = jnp.dot(own_rows, w_key, preferred_element_type=jnp.float32).astype(jnp.bfloat16)
        value_proj = jnp.dot(own_rows, w_value, preferred_element_type=jnp.float32).astype(jnp.bfloat16)
        query_proj = query_proj.reshape(length, HEADS, HEAD_DIM)
        key_proj = key_proj.reshape(length, HEADS, HEAD_DIM)
        value_proj = value_proj.reshape(length, HEADS, HEAD_DIM)
        query_unit = (normalize(query_proj) * qk_gain[0].astype(jnp.float32) * HEAD_DIM ** (-0.5)).astype(jnp.bfloat16)
        key_unit = (normalize(key_proj) * qk_gain[1].astype(jnp.float32)).astype(jnp.bfloat16)
        attended = attend(query_unit, key_unit, value_proj, decay_rows)
        head_out = normalize(attended).astype(jnp.bfloat16).reshape(length, HEADS * HEAD_DIM)
        return jnp.dot(head_out, w_output, preferred_element_type=jnp.float32).astype(jnp.bfloat16)
    return lax.map(one_sequence, (tokens, decay_sums))
```

```python
import functools

import jax
import jax.numpy as jnp
from jax import lax
from jax.experimental import pallas as pl
from jax.experimental.pallas import tpu as pltpu
from jax.sharding import PartitionSpec as P

EPS = 1e-06
DIMS_NT = (((1,), (1,)), ((), ()))


def attention_kernel(
    heads, width, block, rows_ref, weight_ref, gain_ref, decay_ref, out_ref, key_ref, value_ref
):
    index = pl.program_id(0)
    wide = heads * width
    projected = jnp.dot(
        rows_ref[...], weight_ref[...], preferred_element_type=jnp.float32
    ).astype(jnp.bfloat16)
    place = pl.ds(pl.multiple_of(index * block, block), block)

    def unit(values, gain):
        values = values.astype(jnp.float32)
        scale = lax.rsqrt(jnp.mean(values * values, axis=-1, keepdims=True) + EPS)
        return values * scale * gain

    values_turned = projected[:, 2 * wide :].astype(jnp.float32).T
    lane = lax.broadcasted_iota(jnp.int32, (block, width), 1)
    ones_lanes = jnp.where(lane < 3, 1.0, 0.0)
    sub = lax.broadcasted_iota(jnp.int32, (2 * width, block), 0)
    ones_rows = jnp.where(
        lax.broadcasted_iota(jnp.int32, (16, block), 0) == 0, 1.0, 0.0
    )
    queries = []
    for head in range(heads):
        low = head * width
        query = unit(projected[:, low : low + width], gain_ref[0:1, :]) * width ** (-0.5)
        key = unit(projected[:, wide + low : wide + low + width], gain_ref[1:2, :])
        decay = -decay_ref[head : head + 1, :]
        first = decay.astype(jnp.bfloat16).astype(jnp.float32)
        rest = decay - first
        second = rest.astype(jnp.bfloat16).astype(jnp.float32)
        third = rest - second
        parts = jnp.where(
            sub == 0, first, jnp.where(sub == 1, second, jnp.where(sub == 2, third, 0.0))
        ).T
        queries.append(jnp.concatenate([query, ones_lanes], axis=1).astype(jnp.bfloat16))
        key_ref[head, place, :] = jnp.concatenate([key, parts[:, :width]], axis=1).astype(
            jnp.bfloat16
        )
        value_ref[head, index] = jnp.concatenate(
            [values_turned[low : low + width], ones_rows], axis=0
        ).astype(jnp.bfloat16)

    def step(column, carry, masked):
        fresh = []
        for head in range(heads):
            peak, total = carry[head]
            keys = key_ref[head, pl.ds(pl.multiple_of(column * block, block), block), :]
            scores = lax.dot_general(
                keys, queries[head], DIMS_NT, preferred_element_type=jnp.float32
            )
            if masked:
                key_place = lax.broadcasted_iota(jnp.int32, scores.shape, 0)
                query_place = lax.broadcasted_iota(jnp.int32, scores.shape, 1)
                scores = jnp.where(key_place <= query_place, scores, -jnp.inf)
            higher = jnp.maximum(peak, jnp.max(scores, axis=0, keepdims=True))
            probs = jnp.exp(scores - higher).astype(jnp.bfloat16)
            total = total * jnp.exp(peak - higher) + jnp.dot(
                value_ref[head, column], probs, preferred_element_type=jnp.float32
            )
            fresh.append((higher, total))
        return tuple(fresh)

    start = tuple(
        (
            jnp.full((1, block), -1e30, jnp.float32),
            jnp.zeros((width + 16, block), jnp.float32),
        )
        for _ in range(heads)
    )
    carry = step(index, start, True)
    carry = lax.fori_loop(0, index, lambda column, c: step(column, c, False), carry)
    outs = []
    for head in range(heads):
        total = carry[head][1]
        mixed, norm = total[:width], total[width : width + 1]
        scale = lax.rsqrt(jnp.mean(mixed * mixed, axis=0, keepdims=True) + EPS * norm * norm)
        outs.append(mixed * scale)
    out_ref[...] = jnp.concatenate(outs, axis=0).T.astype(jnp.bfloat16)


def attend(whole, weights, qk_gain, decay_rows):
    length, depth = whole.shape
    heads = decay_rows.shape[0]
    width = qk_gain.shape[1]
    block = 512
    steps = length // block
    wide = heads * width
    return pl.pallas_call(
        functools.partial(attention_kernel, heads, width, block),
        grid=(steps,),
        out_shape=jax.ShapeDtypeStruct((length, wide), jnp.bfloat16),
        in_specs=[
            pl.BlockSpec((block, depth), lambda i: (i, 0)),
            pl.BlockSpec((depth, 3 * wide), lambda i: (0, 0)),
            pl.BlockSpec((2, width), lambda i: (0, 0)),
            pl.BlockSpec((heads, block), lambda i: (0, i)),
        ],
        out_specs=pl.BlockSpec((block, wide), lambda i: (i, 0)),
        scratch_shapes=[
            pltpu.VMEM((heads, length, 2 * width), jnp.bfloat16),
            pltpu.VMEM((heads, steps, width + 16, block), jnp.bfloat16),
        ],
        compiler_params=pltpu.CompilerParams(vmem_limit_bytes=56 * 1024 * 1024),
        cost_estimate=pl.CostEstimate(
            flops=2 * length * depth * 3 * wide + 2 * heads * length * length * 2 * width,
            bytes_accessed=2 * length * depth,
            transcendentals=heads * length * length // 2,
        ),
    )(whole, weights, qk_gain, decay_rows)


def on_device(tokens, w_query, w_key, w_value, w_output, qk_gain, decay_sums):
    own_rows = tokens[0]
    stacked = jnp.concatenate((w_query, w_key, w_value), axis=1)
    columns = lax.all_gather(stacked, "dp", axis=0, tiled=True)
    whole = lax.all_gather(own_rows, "sp", axis=0, tiled=True)
    out_rows = lax.all_gather(w_output, "sp", axis=0, tiled=True)
    out_weight = lax.all_gather(out_rows, "dp", axis=1, tiled=True)
    head_out = attend(whole, columns, qk_gain, decay_sums[0])
    merged = lax.all_to_all(head_out, "sp", split_axis=0, concat_axis=1, tiled=True)
    result = jnp.dot(merged, out_weight, preferred_element_type=jnp.float32)
    return result.astype(jnp.bfloat16)[None]


def solution(mesh):
    placed = (
        P("dp", "sp", None),
        P("dp", "sp"),
        P("dp", "sp"),
        P("dp", "sp"),
        P("sp", "dp"),
        P(),
        P("dp", "sp", None),
    )
    return jax.shard_map(
        on_device, mesh=mesh, in_specs=placed, out_specs=P("dp", "sp", None), check_vma=False
    )
```

```python
import functools

import jax
import jax.numpy as jnp
from jax import lax
from jax.experimental import pallas as pl
from jax.experimental.pallas import tpu as pltpu
from jax.sharding import PartitionSpec as P

EPS = 1e-06
DIMS_NT = (((1,), (1,)), ((), ()))


def attention_kernel(
    heads, width, block, rows_ref, weight_ref, gain_ref, decay_ref, out_ref, key_ref, value_ref
):
    index = pl.program_id(0)
    wide = heads * width
    place = pl.ds(pl.multiple_of(index * block, block), block)
    projected = jnp.dot(
        rows_ref[place, :], weight_ref[...], preferred_element_type=jnp.float32
    ).astype(jnp.bfloat16)

    def unit(values, gain):
        values = values.astype(jnp.float32)
        scale = lax.rsqrt(jnp.mean(values * values, axis=-1, keepdims=True) + EPS)
        return values * scale * gain

    values_turned = projected[:, 2 * wide :].astype(jnp.float32).T
    lane = lax.broadcasted_iota(jnp.int32, (block, width), 1)
    ones_lanes = jnp.where(lane < 3, 1.0, 0.0)
    sub = lax.broadcasted_iota(jnp.int32, (2 * width, block), 0)
    ones_rows = jnp.where(
        lax.broadcasted_iota(jnp.int32, (16, block), 0) == 0, 1.0, 0.0
    )
    queries = []
    for head in range(heads):
        low = head * width
        query = unit(projected[:, low : low + width], gain_ref[0:1, :]) * width ** (-0.5)
        key = unit(projected[:, wide + low : wide + low + width], gain_ref[1:2, :])
        decay = -decay_ref[head : head + 1, :]
        first = decay.astype(jnp.bfloat16).astype(jnp.float32)
        rest = decay - first
        second = rest.astype(jnp.bfloat16).astype(jnp.float32)
        third = rest - second
        parts = jnp.where(
            sub == 0, first, jnp.where(sub == 1, second, jnp.where(sub == 2, third, 0.0))
        ).T
        queries.append(jnp.concatenate([query, ones_lanes], axis=1).astype(jnp.bfloat16))
        key_ref[head, place, :] = jnp.concatenate([key, parts[:, :width]], axis=1).astype(
            jnp.bfloat16
        )
        value_ref[head, index] = jnp.concatenate(
            [values_turned[low : low + width], ones_rows], axis=0
        ).astype(jnp.bfloat16)

    def step(column, carry, masked):
        fresh = []
        for head in range(heads):
            peak, total = carry[head]
            keys = key_ref[head, pl.ds(pl.multiple_of(column * block, block), block), :]
            scores = lax.dot_general(
                keys, queries[head], DIMS_NT, preferred_element_type=jnp.float32
            )
            if masked:
                key_place = lax.broadcasted_iota(jnp.int32, scores.shape, 0)
                query_place = lax.broadcasted_iota(jnp.int32, scores.shape, 1)
                scores = jnp.where(key_place <= query_place, scores, -jnp.inf)
            higher = jnp.maximum(peak, jnp.max(scores, axis=0, keepdims=True))
            probs = jnp.exp(scores - higher).astype(jnp.bfloat16)
            total = total * jnp.exp(peak - higher) + jnp.dot(
                value_ref[head, column], probs, preferred_element_type=jnp.float32
            )
            fresh.append((higher, total))
        return tuple(fresh)

    start = tuple(
        (
            jnp.full((1, block), -1e30, jnp.float32),
            jnp.zeros((width + 16, block), jnp.float32),
        )
        for _ in range(heads)
    )
    carry = step(index, start, True)
    carry = lax.fori_loop(0, index, lambda column, c: step(column, c, False), carry)
    outs = []
    for head in range(heads):
        total = carry[head][1]
        mixed, norm = total[:width], total[width : width + 1]
        scale = lax.rsqrt(jnp.mean(mixed * mixed, axis=0, keepdims=True) + EPS * norm * norm)
        outs.append(mixed * scale)
    out_ref[...] = jnp.concatenate(outs, axis=0).T.astype(jnp.bfloat16)


def attend(whole, weights, qk_gain, decay_rows):
    length, depth = whole.shape
    heads = decay_rows.shape[0]
    width = qk_gain.shape[1]
    block = 512
    steps = length // block
    wide = heads * width
    return pl.pallas_call(
        functools.partial(attention_kernel, heads, width, block),
        grid=(steps,),
        out_shape=jax.ShapeDtypeStruct((length, wide), jnp.bfloat16),
        in_specs=[
            pl.BlockSpec(memory_space=pltpu.VMEM),
            pl.BlockSpec((depth, 3 * wide), lambda i: (0, 0)),
            pl.BlockSpec((2, width), lambda i: (0, 0)),
            pl.BlockSpec((heads, block), lambda i: (0, i)),
        ],
        out_specs=pl.BlockSpec((block, wide), lambda i: (i, 0)),
        scratch_shapes=[
            pltpu.VMEM((heads, length, 2 * width), jnp.bfloat16),
            pltpu.VMEM((heads, steps, width + 16, block), jnp.bfloat16),
        ],
        compiler_params=pltpu.CompilerParams(vmem_limit_bytes=44 * 1024 * 1024),
        cost_estimate=pl.CostEstimate(
            flops=2 * length * depth * 3 * wide + 2 * heads * length * length * 2 * width,
            bytes_accessed=2 * length * depth,
            transcendentals=heads * length * length // 2,
        ),
    )(whole, weights, qk_gain, decay_rows)


PIECES = 2


def ring_kernel(count, own_ref, whole_ref, send_sem, recv_sem, local_sem):
    rows = own_ref.shape[0]
    part = rows // (2 * PIECES)
    tall = 4 if count % 4 == 0 else 1
    broad = count // tall

    def member(spot):
        spot = lax.rem(spot + 2 * count, count)
        column, height = spot // tall, lax.rem(spot, tall)
        level = height + lax.rem(column, 2) * (tall - 1 - 2 * height)
        return level * broad + column

    me = lax.axis_index("sp")
    level, column = me // broad, lax.rem(me, broad)
    spot = column * tall + level + lax.rem(column, 2) * (tall - 1 - 2 * level)
    ways = (1, -1)
    targets = [member(spot + way) for way in ways]

    barrier = pltpu.get_barrier_semaphore()
    for target in targets:
        pl.semaphore_signal(
            barrier, inc=1, device_id={"sp": target}, device_id_type=pl.DeviceIdType.MESH
        )
    pl.semaphore_wait(barrier, 2)

    local = pltpu.make_async_copy(
        own_ref, whole_ref.at[pl.ds(pl.multiple_of(me * rows, rows), rows)], local_sem
    )
    local.start()
    copies = {}
    for step in range(count - 1):
        for piece in range(PIECES):
            for side, way in enumerate(ways):
                offset = (side * PIECES + piece) * part
                if step:
                    copies[step - 1, piece, side].wait_recv()
                origin = member(spot - way * step)
                place = pl.ds(pl.multiple_of(origin * rows + offset, part), part)
                source = own_ref.at[pl.ds(offset, part)] if step == 0 else whole_ref.at[place]
                copy = pltpu.make_async_remote_copy(
                    src_ref=source,
                    dst_ref=whole_ref.at[place],
                    send_sem=send_sem.at[step, piece, side],
                    recv_sem=recv_sem.at[step, piece, side],
                    device_id={"sp": targets[side]},
                    device_id_type=pl.DeviceIdType.MESH,
                )
                copy.start()
                copies[step, piece, side] = copy
    for piece in range(PIECES):
        for side in range(2):
            copies[count - 2, piece, side].wait_recv()
    for copy in copies.values():
        copy.wait_send()
    local.wait()


def gather_rows(own_rows, count):
    rows, depth = own_rows.shape
    shape = (count - 1, PIECES, 2)
    return pl.pallas_call(
        functools.partial(ring_kernel, count),
        out_shape=jax.ShapeDtypeStruct((count * rows, depth), own_rows.dtype),
        in_specs=[pl.BlockSpec(memory_space=pltpu.VMEM)],
        out_specs=pl.BlockSpec(memory_space=pl.ANY),
        scratch_shapes=[
            pltpu.SemaphoreType.DMA(shape),
            pltpu.SemaphoreType.DMA(shape),
            pltpu.SemaphoreType.DMA,
        ],
        compiler_params=pltpu.CompilerParams(
            collective_id=0, has_side_effects=True, vmem_limit_bytes=16 * 1024 * 1024
        ),
        cost_estimate=pl.CostEstimate(
            flops=10**11, bytes_accessed=2 * count * rows * depth, transcendentals=0
        ),
    )(own_rows)


def on_device(tokens, w_query, w_key, w_value, w_output, qk_gain, decay_sums):
    own_rows = tokens[0]
    stacked = jnp.concatenate((w_query, w_key, w_value), axis=1)
    columns = lax.all_gather(stacked, "dp", axis=0, tiled=True)
    whole = gather_rows(own_rows, lax.axis_size("sp"))
    out_rows = lax.all_gather(w_output, "sp", axis=0, tiled=True)
    whole, out_rows = lax.optimization_barrier((whole, out_rows))
    out_weight = lax.all_gather(out_rows, "dp", axis=1, tiled=True)
    head_out = attend(whole, columns, qk_gain, decay_sums[0])
    merged = lax.all_to_all(head_out, "sp", split_axis=0, concat_axis=1, tiled=True)
    result = jnp.dot(merged, out_weight, preferred_element_type=jnp.float32)
    return result.astype(jnp.bfloat16)[None]


def solution(mesh):
    placed = (
        P("dp", "sp", None),
        P("dp", "sp"),
        P("dp", "sp"),
        P("dp", "sp"),
        P("sp", "dp"),
        P(),
        P("dp", "sp", None),
    )
    return jax.shard_map(
        on_device, mesh=mesh, in_specs=placed, out_specs=P("dp", "sp", None), check_vma=False
    )
```

```python
import functools

import jax
import jax.numpy as jnp
from jax import lax
from jax.experimental import pallas as pl
from jax.experimental.pallas import tpu as pltpu
from jax.sharding import PartitionSpec as P

EPS = 1e-06
DIMS_NT = (((1,), (1,)), ((), ()))


def attention_kernel(
    heads,
    width,
    block,
    count,
    rows_ref,
    weight_ref,
    gain_ref,
    decay_ref,
    merged_ref,
    key_ref,
    value_ref,
    done_ref,
    send_sem,
    recv_sem,
    local_sem,
):
    index = pl.program_id(0)
    me = lax.axis_index("sp")
    rows = merged_ref.shape[1]
    owners = block // rows

    @pl.when(index == 0)
    def _():
        barrier = pltpu.get_barrier_semaphore()
        for shift in range(1, count):
            pl.semaphore_signal(
                barrier,
                inc=1,
                device_id={"sp": lax.rem(me + shift, count)},
                device_id_type=pl.DeviceIdType.MESH,
            )
        pl.semaphore_wait(barrier, count - 1)

    wide = heads * width
    place = pl.ds(pl.multiple_of(index * block, block), block)
    projected = jnp.dot(
        rows_ref[place, :], weight_ref[...], preferred_element_type=jnp.float32
    ).astype(jnp.bfloat16)

    def unit(values, gain):
        values = values.astype(jnp.float32)
        scale = lax.rsqrt(jnp.mean(values * values, axis=-1, keepdims=True) + EPS)
        return values * scale * gain

    values_turned = projected[:, 2 * wide :].astype(jnp.float32).T
    lane = lax.broadcasted_iota(jnp.int32, (block, width), 1)
    ones_lanes = jnp.where(lane < 3, 1.0, 0.0)
    sub = lax.broadcasted_iota(jnp.int32, (2 * width, block), 0)
    ones_rows = jnp.where(
        lax.broadcasted_iota(jnp.int32, (16, block), 0) == 0, 1.0, 0.0
    )
    queries = []
    for head in range(heads):
        low = head * width
        query = unit(projected[:, low : low + width], gain_ref[0:1, :]) * width ** (-0.5)
        key = unit(projected[:, wide + low : wide + low + width], gain_ref[1:2, :])
        decay = -decay_ref[head : head + 1, :]
        first = decay.astype(jnp.bfloat16).astype(jnp.float32)
        rest = decay - first
        second = rest.astype(jnp.bfloat16).astype(jnp.float32)
        third = rest - second
        parts = jnp.where(
            sub == 0, first, jnp.where(sub == 1, second, jnp.where(sub == 2, third, 0.0))
        ).T
        queries.append(jnp.concatenate([query, ones_lanes], axis=1).astype(jnp.bfloat16))
        key_ref[head, place, :] = jnp.concatenate([key, parts[:, :width]], axis=1).astype(
            jnp.bfloat16
        )
        value_ref[head, index] = jnp.concatenate(
            [values_turned[low : low + width], ones_rows], axis=0
        ).astype(jnp.bfloat16)

    def step(column, carry, masked):
        fresh = []
        for head in range(heads):
            peak, total = carry[head]
            keys = key_ref[head, pl.ds(pl.multiple_of(column * block, block), block), :]
            scores = lax.dot_general(
                keys, queries[head], DIMS_NT, preferred_element_type=jnp.float32
            )
            if masked:
                key_place = lax.broadcasted_iota(jnp.int32, scores.shape, 0)
                query_place = lax.broadcasted_iota(jnp.int32, scores.shape, 1)
                scores = jnp.where(key_place <= query_place, scores, -jnp.inf)
            higher = jnp.maximum(peak, jnp.max(scores, axis=0, keepdims=True))
            probs = jnp.exp(scores - higher).astype(jnp.bfloat16)
            total = total * jnp.exp(peak - higher) + jnp.dot(
                value_ref[head, column], probs, preferred_element_type=jnp.float32
            )
            fresh.append((higher, total))
        return tuple(fresh)

    start = tuple(
        (
            jnp.full((1, block), -1e30, jnp.float32),
            jnp.zeros((width + 16, block), jnp.float32),
        )
        for _ in range(heads)
    )
    carry = step(index, start, True)
    carry = lax.fori_loop(0, index, lambda column, c: step(column, c, False), carry)
    outs = []
    for head in range(heads):
        total = carry[head][1]
        mixed, norm = total[:width], total[width : width + 1]
        scale = lax.rsqrt(jnp.mean(mixed * mixed, axis=0, keepdims=True) + EPS * norm * norm)
        outs.append(mixed * scale)
    turned = jnp.concatenate(outs, axis=0).T.astype(jnp.bfloat16)
    for part in range(owners):
        done_ref[index * owners + part] = turned[part * rows : (part + 1) * rows]

    def remote(source, owner):
        return pltpu.make_async_remote_copy(
            src_ref=done_ref.at[owner],
            dst_ref=merged_ref.at[source],
            send_sem=send_sem.at[owner],
            recv_sem=recv_sem.at[source],
            device_id={"sp": owner},
            device_id_type=pl.DeviceIdType.MESH,
        )

    def local():
        return pltpu.make_async_copy(done_ref.at[me], merged_ref.at[me], local_sem)

    for part in range(owners):
        owner = index * owners + part

        @pl.when(owner != me)
        def _():
            remote(me, owner).start()

        @pl.when(owner == me)
        def _():
            local().start()

    @pl.when(index == pl.num_programs(0) - 1)
    def _():
        for shift in range(1, count):
            other = lax.rem(me + shift, count)
            remote(other, other).wait_recv()
            remote(me, other).wait_send()
        local().wait()


def attend(whole, weights, qk_gain, decay_rows, rows):
    length, depth = whole.shape
    heads = decay_rows.shape[0]
    width = qk_gain.shape[1]
    block = 2 * rows
    steps = length // block
    count = length // rows
    wide = heads * width
    return pl.pallas_call(
        functools.partial(attention_kernel, heads, width, block, count),
        grid=(steps,),
        out_shape=jax.ShapeDtypeStruct((count, rows, wide), jnp.bfloat16),
        in_specs=[
            pl.BlockSpec(memory_space=pltpu.VMEM),
            pl.BlockSpec((depth, 3 * wide), lambda i: (0, 0)),
            pl.BlockSpec((2, width), lambda i: (0, 0)),
            pl.BlockSpec((heads, block), lambda i: (0, i)),
        ],
        out_specs=pl.BlockSpec(memory_space=pl.ANY),
        scratch_shapes=[
            pltpu.VMEM((heads, length, 2 * width), jnp.bfloat16),
            pltpu.VMEM((heads, steps, width + 16, block), jnp.bfloat16),
            pltpu.VMEM((count, rows, wide), jnp.bfloat16),
            pltpu.SemaphoreType.DMA((count,)),
            pltpu.SemaphoreType.DMA((count,)),
            pltpu.SemaphoreType.DMA,
        ],
        compiler_params=pltpu.CompilerParams(
            collective_id=1, has_side_effects=True, vmem_limit_bytes=40 * 1024 * 1024
        ),
        cost_estimate=pl.CostEstimate(
            flops=2 * length * depth * 3 * wide + 2 * heads * length * length * 2 * width,
            bytes_accessed=2 * length * depth,
            transcendentals=heads * length * length // 2,
        ),
    )(whole, weights, qk_gain, decay_rows)


PIECES = 2


def ring_kernel(count, own_ref, whole_ref, mark_ref, send_sem, recv_sem, local_sem):
    rows = own_ref.shape[0]
    part = rows // (2 * PIECES)
    tall = 4 if count % 4 == 0 else 1
    broad = count // tall

    def member(spot):
        spot = lax.rem(spot + 2 * count, count)
        column, height = spot // tall, lax.rem(spot, tall)
        level = height + lax.rem(column, 2) * (tall - 1 - 2 * height)
        return level * broad + column

    me = lax.axis_index("sp")
    level, column = me // broad, lax.rem(me, broad)
    spot = column * tall + level + lax.rem(column, 2) * (tall - 1 - 2 * level)
    ways = (1, -1)
    targets = [member(spot + way) for way in ways]

    barrier = pltpu.get_barrier_semaphore()
    for target in targets:
        pl.semaphore_signal(
            barrier, inc=1, device_id={"sp": target}, device_id_type=pl.DeviceIdType.MESH
        )
    pl.semaphore_wait(barrier, 2)

    local = pltpu.make_async_copy(
        own_ref, whole_ref.at[pl.ds(pl.multiple_of(me * rows, rows), rows)], local_sem
    )
    local.start()
    copies = {}
    for step in range(count - 1):
        for piece in range(PIECES):
            for side, way in enumerate(ways):
                offset = (side * PIECES + piece) * part
                if step:
                    copies[step - 1, piece, side].wait_recv()
                origin = member(spot - way * step)
                place = pl.ds(pl.multiple_of(origin * rows + offset, part), part)
                source = own_ref.at[pl.ds(offset, part)] if step == 0 else whole_ref.at[place]
                copy = pltpu.make_async_remote_copy(
                    src_ref=source,
                    dst_ref=whole_ref.at[place],
                    send_sem=send_sem.at[step, piece, side],
                    recv_sem=recv_sem.at[step, piece, side],
                    device_id={"sp": targets[side]},
                    device_id_type=pl.DeviceIdType.MESH,
                )
                copy.start()
                copies[step, piece, side] = copy
    for piece in range(PIECES):
        for side in range(2):
            copies[count - 2, piece, side].wait_recv()
    for copy in copies.values():
        copy.wait_send()
    local.wait()
    mark_ref[...] = jnp.zeros_like(mark_ref)


def gather_rows(own_rows, count):
    rows, depth = own_rows.shape
    shape = (count - 1, PIECES, 2)
    return pl.pallas_call(
        functools.partial(ring_kernel, count),
        out_shape=(
            jax.ShapeDtypeStruct((count * rows, depth), own_rows.dtype),
            jax.ShapeDtypeStruct((8, 128), jnp.float32),
        ),
        in_specs=[pl.BlockSpec(memory_space=pltpu.VMEM)],
        out_specs=(pl.BlockSpec(memory_space=pl.ANY), pl.BlockSpec(memory_space=pltpu.VMEM)),
        scratch_shapes=[
            pltpu.SemaphoreType.DMA(shape),
            pltpu.SemaphoreType.DMA(shape),
            pltpu.SemaphoreType.DMA,
        ],
        compiler_params=pltpu.CompilerParams(
            collective_id=0, has_side_effects=True, vmem_limit_bytes=16 * 1024 * 1024
        ),
        cost_estimate=pl.CostEstimate(
            flops=10**11, bytes_accessed=2 * count * rows * depth, transcendentals=0
        ),
    )(own_rows)


def on_device(tokens, w_query, w_key, w_value, w_output, qk_gain, decay_sums):
    own_rows = tokens[0]
    stacked = jnp.concatenate((w_query, w_key, w_value), axis=1)
    columns = lax.all_gather(stacked, "dp", axis=0, tiled=True)
    whole, mark = gather_rows(own_rows, lax.axis_size("sp"))
    out_rows = lax.all_gather(w_output, "sp", axis=0, tiled=True)
    mark, out_rows = lax.optimization_barrier((mark, out_rows))
    out_weight = lax.all_gather(out_rows, "dp", axis=1, tiled=True)
    merged = attend(whole, columns, qk_gain, decay_sums[0], own_rows.shape[0])
    merged = merged.transpose(1, 0, 2).reshape(own_rows.shape[0], -1)
    result = jnp.dot(merged, out_weight, preferred_element_type=jnp.float32)
    return result.astype(jnp.bfloat16)[None]


def solution(mesh):
    placed = (
        P("dp", "sp", None),
        P("dp", "sp"),
        P("dp", "sp"),
        P("dp", "sp"),
        P("sp", "dp"),
        P(),
        P("dp", "sp", None),
    )
    return jax.shard_map(
        on_device, mesh=mesh, in_specs=placed, out_specs=P("dp", "sp", None), check_vma=False
    )
```

```python
import functools

import jax
import jax.numpy as jnp
from jax import lax
from jax.experimental import pallas as pl
from jax.experimental.pallas import tpu as pltpu
from jax.sharding import PartitionSpec as P

EPS = 1e-06
DIMS_NT = (((1,), (1,)), ((), ()))


def attention_kernel(
    heads,
    width,
    block,
    count,
    rows_ref,
    weight_ref,
    gain_ref,
    decay_ref,
    merged_ref,
    key_ref,
    value_ref,
    done_ref,
    send_sem,
    recv_sem,
    local_sem,
):
    index = pl.program_id(0)
    me = lax.axis_index("sp")
    rows = merged_ref.shape[1]
    owners = block // rows

    @pl.when(index == 0)
    def _():
        barrier = pltpu.get_barrier_semaphore()
        for shift in range(1, count):
            pl.semaphore_signal(
                barrier,
                inc=1,
                device_id={"sp": lax.rem(me + shift, count)},
                device_id_type=pl.DeviceIdType.MESH,
            )
        pl.semaphore_wait(barrier, count - 1)

    wide = heads * width
    place = pl.ds(pl.multiple_of(index * block, block), block)
    projected = jnp.dot(
        rows_ref[...], weight_ref[...], preferred_element_type=jnp.float32
    ).astype(jnp.bfloat16)

    def unit(values, gain):
        values = values.astype(jnp.float32)
        scale = lax.rsqrt(jnp.mean(values * values, axis=-1, keepdims=True) + EPS)
        return values * scale * gain

    values_turned = projected[:, 2 * wide :].astype(jnp.float32).T
    lane = lax.broadcasted_iota(jnp.int32, (block, width), 1)
    ones_lanes = jnp.where(lane < 3, 1.0, 0.0)
    sub = lax.broadcasted_iota(jnp.int32, (2 * width, block), 0)
    ones_rows = jnp.where(
        lax.broadcasted_iota(jnp.int32, (16, block), 0) == 0, 1.0, 0.0
    )
    queries = []
    for head in range(heads):
        low = head * width
        query = unit(projected[:, low : low + width], gain_ref[0:1, :]) * width ** (-0.5)
        key = unit(projected[:, wide + low : wide + low + width], gain_ref[1:2, :])
        decay = -decay_ref[head : head + 1, :]
        first = decay.astype(jnp.bfloat16).astype(jnp.float32)
        rest = decay - first
        second = rest.astype(jnp.bfloat16).astype(jnp.float32)
        third = rest - second
        parts = jnp.where(
            sub == 0, first, jnp.where(sub == 1, second, jnp.where(sub == 2, third, 0.0))
        ).T
        queries.append(jnp.concatenate([query, ones_lanes], axis=1).astype(jnp.bfloat16))
        key_ref[head, place, :] = jnp.concatenate([key, parts[:, :width]], axis=1).astype(
            jnp.bfloat16
        )
        value_ref[head, index] = jnp.concatenate(
            [values_turned[low : low + width], ones_rows], axis=0
        ).astype(jnp.bfloat16)

    def step(column, carry, masked):
        fresh = []
        for head in range(heads):
            peak, total = carry[head]
            keys = key_ref[head, pl.ds(pl.multiple_of(column * block, block), block), :]
            scores = lax.dot_general(
                keys, queries[head], DIMS_NT, preferred_element_type=jnp.float32
            )
            if masked:
                key_place = lax.broadcasted_iota(jnp.int32, scores.shape, 0)
                query_place = lax.broadcasted_iota(jnp.int32, scores.shape, 1)
                scores = jnp.where(key_place <= query_place, scores, -jnp.inf)
            higher = jnp.maximum(peak, jnp.max(scores, axis=0, keepdims=True))
            probs = jnp.exp(scores - higher).astype(jnp.bfloat16)
            total = total * jnp.exp(peak - higher) + jnp.dot(
                value_ref[head, column], probs, preferred_element_type=jnp.float32
            )
            fresh.append((higher, total))
        return tuple(fresh)

    start = tuple(
        (
            jnp.full((1, block), -1e30, jnp.float32),
            jnp.zeros((width + 16, block), jnp.float32),
        )
        for _ in range(heads)
    )
    carry = step(index, start, True)
    carry = lax.fori_loop(0, index, lambda column, c: step(column, c, False), carry)
    outs = []
    for head in range(heads):
        total = carry[head][1]
        mixed, norm = total[:width], total[width : width + 1]
        scale = lax.rsqrt(jnp.mean(mixed * mixed, axis=0, keepdims=True) + EPS * norm * norm)
        outs.append(mixed * scale)
    turned = jnp.concatenate(outs, axis=0).T.astype(jnp.bfloat16)
    for part in range(owners):
        done_ref[index * owners + part] = turned[part * rows : (part + 1) * rows]

    def remote(source, owner):
        return pltpu.make_async_remote_copy(
            src_ref=done_ref.at[owner],
            dst_ref=merged_ref.at[source],
            send_sem=send_sem.at[owner],
            recv_sem=recv_sem.at[source],
            device_id={"sp": owner},
            device_id_type=pl.DeviceIdType.MESH,
        )

    def local():
        return pltpu.make_async_copy(done_ref.at[me], merged_ref.at[me], local_sem)

    for part in range(owners):
        owner = index * owners + part

        @pl.when(owner != me)
        def _():
            remote(me, owner).start()

        @pl.when(owner == me)
        def _():
            local().start()

    @pl.when(index == pl.num_programs(0) - 1)
    def _():
        for shift in range(1, count):
            other = lax.rem(me + shift, count)
            remote(other, other).wait_recv()
            remote(me, other).wait_send()
        local().wait()


def attend(whole, weights, qk_gain, decay_rows, rows):
    length, depth = whole.shape
    heads = decay_rows.shape[0]
    width = qk_gain.shape[1]
    block = 2 * rows
    steps = length // block
    count = length // rows
    wide = heads * width
    return pl.pallas_call(
        functools.partial(attention_kernel, heads, width, block, count),
        grid=(steps,),
        out_shape=jax.ShapeDtypeStruct((count, rows, wide), jnp.bfloat16),
        in_specs=[
            pl.BlockSpec((block, depth), lambda i: (i, 0)),
            pl.BlockSpec((depth, 3 * wide), lambda i: (0, 0)),
            pl.BlockSpec((2, width), lambda i: (0, 0)),
            pl.BlockSpec((heads, block), lambda i: (0, i)),
        ],
        out_specs=pl.BlockSpec(memory_space=pl.ANY),
        scratch_shapes=[
            pltpu.VMEM((heads, length, 2 * width), jnp.bfloat16),
            pltpu.VMEM((heads, steps, width + 16, block), jnp.bfloat16),
            pltpu.VMEM((count, rows, wide), jnp.bfloat16),
            pltpu.SemaphoreType.DMA((count,)),
            pltpu.SemaphoreType.DMA((count,)),
            pltpu.SemaphoreType.DMA,
        ],
        compiler_params=pltpu.CompilerParams(
            collective_id=1, has_side_effects=True, vmem_limit_bytes=40 * 1024 * 1024
        ),
        cost_estimate=pl.CostEstimate(
            flops=2 * length * depth * 3 * wide + 2 * heads * length * length * 2 * width,
            bytes_accessed=2 * length * depth,
            transcendentals=heads * length * length // 2,
        ),
    )(whole, weights, qk_gain, decay_rows)


PIECES = 2


def ring_kernel(
    count, own_ref, slab_ref, whole_ref, slabs_ref, send_sem, recv_sem, slab_send, slab_recv, local_sem
):
    rows = own_ref.shape[0]
    part = rows // (2 * PIECES)
    tall = 4 if count % 4 == 0 else 1
    broad = count // tall

    def member(spot):
        spot = lax.rem(spot + 2 * count, count)
        column, height = spot // tall, lax.rem(spot, tall)
        level = height + lax.rem(column, 2) * (tall - 1 - 2 * height)
        return level * broad + column

    me = lax.axis_index("sp")
    level, column = me // broad, lax.rem(me, broad)
    spot = column * tall + level + lax.rem(column, 2) * (tall - 1 - 2 * level)
    ways = (1, -1)
    targets = [member(spot + way) for way in ways]

    barrier = pltpu.get_barrier_semaphore()
    for target in targets:
        pl.semaphore_signal(
            barrier, inc=1, device_id={"sp": target}, device_id_type=pl.DeviceIdType.MESH
        )
    pl.semaphore_wait(barrier, 2)

    local = pltpu.make_async_copy(
        own_ref, whole_ref.at[pl.ds(pl.multiple_of(me * rows, rows), rows)], local_sem.at[0]
    )
    local.start()
    tall_slab = slab_ref.shape[0]
    half = tall_slab // 2
    local_slab = pltpu.make_async_copy(
        slab_ref,
        slabs_ref.at[pl.ds(pl.multiple_of(me * tall_slab, tall_slab), tall_slab)],
        local_sem.at[1],
    )
    local_slab.start()
    copies = {}
    for step in range(count - 1):
        for piece in range(PIECES):
            for side, way in enumerate(ways):
                offset = (side * PIECES + piece) * part
                if step:
                    copies[step - 1, piece, side].wait_recv()
                origin = member(spot - way * step)
                place = pl.ds(pl.multiple_of(origin * rows + offset, part), part)
                source = own_ref.at[pl.ds(offset, part)] if step == 0 else whole_ref.at[place]
                copy = pltpu.make_async_remote_copy(
                    src_ref=source,
                    dst_ref=whole_ref.at[place],
                    send_sem=send_sem.at[step, piece, side],
                    recv_sem=recv_sem.at[step, piece, side],
                    device_id={"sp": targets[side]},
                    device_id_type=pl.DeviceIdType.MESH,
                )
                copy.start()
                copies[step, piece, side] = copy
        for side, way in enumerate(ways):
            if step:
                copies[step - 1, "slab", side].wait_recv()
            origin = member(spot - way * step)
            place = pl.ds(pl.multiple_of(origin * tall_slab + side * half, half), half)
            source = slab_ref.at[pl.ds(side * half, half)] if step == 0 else slabs_ref.at[place]
            copy = pltpu.make_async_remote_copy(
                src_ref=source,
                dst_ref=slabs_ref.at[place],
                send_sem=slab_send.at[step, side],
                recv_sem=slab_recv.at[step, side],
                device_id={"sp": targets[side]},
                device_id_type=pl.DeviceIdType.MESH,
            )
            copy.start()
            copies[step, "slab", side] = copy
    for piece in (*range(PIECES), "slab"):
        for side in range(2):
            copies[count - 2, piece, side].wait_recv()
    for copy in copies.values():
        copy.wait_send()
    local.wait()
    local_slab.wait()


def gather_rows(own_rows, slab, count):
    rows, depth = own_rows.shape
    shape = (count - 1, PIECES, 2)
    return pl.pallas_call(
        functools.partial(ring_kernel, count),
        out_shape=(
            jax.ShapeDtypeStruct((count * rows, depth), own_rows.dtype),
            jax.ShapeDtypeStruct((count * slab.shape[0], slab.shape[1]), slab.dtype),
        ),
        in_specs=[pl.BlockSpec(memory_space=pltpu.VMEM)] * 2,
        out_specs=(pl.BlockSpec(memory_space=pltpu.HBM), pl.BlockSpec(memory_space=pltpu.HBM)),
        scratch_shapes=[
            pltpu.SemaphoreType.DMA(shape),
            pltpu.SemaphoreType.DMA(shape),
            pltpu.SemaphoreType.DMA((count - 1, 2)),
            pltpu.SemaphoreType.DMA((count - 1, 2)),
            pltpu.SemaphoreType.DMA((2,)),
        ],
        compiler_params=pltpu.CompilerParams(
            collective_id=0, has_side_effects=True, vmem_limit_bytes=16 * 1024 * 1024
        ),
        cost_estimate=pl.CostEstimate(
            flops=10**11, bytes_accessed=2 * count * rows * depth, transcendentals=0
        ),
    )(own_rows, slab)


def on_device(tokens, w_query, w_key, w_value, w_output, qk_gain, decay_sums):
    own_rows = tokens[0]
    stacked = jnp.concatenate((w_query, w_key, w_value), axis=1)
    columns = lax.all_gather(stacked, "dp", axis=0, tiled=True)
    whole, out_rows = gather_rows(own_rows, w_output, lax.axis_size("sp"))
    out_weight = lax.all_gather(out_rows, "dp", axis=1, tiled=True)
    merged = attend(whole, columns, qk_gain, decay_sums[0], own_rows.shape[0])
    merged = merged.transpose(1, 0, 2).reshape(own_rows.shape[0], -1)
    result = jnp.dot(merged, out_weight, preferred_element_type=jnp.float32)
    return result.astype(jnp.bfloat16)[None]


def solution(mesh):
    placed = (
        P("dp", "sp", None),
        P("dp", "sp"),
        P("dp", "sp"),
        P("dp", "sp"),
        P("sp", "dp"),
        P(),
        P("dp", "sp", None),
    )
    return jax.shard_map(
        on_device, mesh=mesh, in_specs=placed, out_specs=P("dp", "sp", None), check_vma=False
    )
```

```python
import functools

import jax
import jax.numpy as jnp
from jax import lax
from jax.experimental import pallas as pl
from jax.experimental.pallas import tpu as pltpu
from jax.sharding import PartitionSpec as P

EPS = 1e-06
DIMS_NT = (((1,), (1,)), ((), ()))


PIECES = 2
MESH = pl.DeviceIdType.MESH


def layer_kernel(
    heads, width, count, groups,
    own_ref, stacked_ref, slab_ref, gain_ref, decay_ref, out_ref,
    whole_ref, weight_ref, slabs_ref, projected_ref, key_ref, value_ref, done_ref, merged_ref,
    send_sem, recv_sem, slab_send, slab_recv, pass_send, pass_recv, weight_send, weight_recv,
    done_send, done_recv,
):
    rows, depth = own_ref.shape
    owners = 2
    block = owners * rows
    wide = heads * width
    part = rows // (2 * PIECES)
    tall = 4 if count % 4 == 0 else 1
    broad = count // tall
    me, group = lax.axis_index("sp"), lax.axis_index("dp")

    def member(spot):
        spot = lax.rem(spot + 2 * count, count)
        column, height = spot // tall, lax.rem(spot, tall)
        level = height + lax.rem(column, 2) * (tall - 1 - 2 * height)
        return level * broad + column

    level, column = me // broad, lax.rem(me, broad)
    spot = column * tall + level + lax.rem(column, 2) * (tall - 1 - 2 * level)
    ways = (1, -1)
    targets = [member(spot + way) for way in ways]
    peers = [lax.rem(group + shift, groups) for shift in range(1, groups)]

    barrier = pltpu.get_barrier_semaphore()
    for shift in range(1, count):
        other = lax.rem(me + shift, count)
        pl.semaphore_signal(barrier, inc=1, device_id={"sp": other}, device_id_type=MESH)
    for peer in peers:
        pl.semaphore_signal(barrier, inc=1, device_id={"dp": peer}, device_id_type=MESH)
    pl.semaphore_wait(barrier, count + groups - 2)

    def send(source, target, out_sem, in_sem, device):
        copy = pltpu.make_async_remote_copy(
            src_ref=source, dst_ref=target, send_sem=out_sem, recv_sem=in_sem,
            device_id=device, device_id_type=MESH,
        )
        copy.start()
        return copy

    tall_slab = slab_ref.shape[0]
    half = tall_slab // 2
    copies, passed, weights, backlog = {}, [], [], []

    def slab_place(origin, side):
        return pl.ds(pl.multiple_of(origin * tall_slab + side * half, half), half)

    def pass_on(step, side, source, place):
        for number, peer in enumerate(peers):
            passed.append(
                send(
                    source, slabs_ref.at[group, place], pass_send.at[number, step, side],
                    pass_recv.at[number, step, side], {"dp": peer},
                )
            )

    def project(place):
        projected_ref[place, :] = jnp.dot(
            whole_ref[place, :], weight_ref[...].reshape(depth, 3 * wide),
            preferred_element_type=jnp.float32,
        ).astype(jnp.bfloat16)

    for step in range(count):
        arrived = []
        for piece in range(PIECES):
            for side, way in enumerate(ways):
                offset = (side * PIECES + piece) * part
                if step:
                    copies[step - 1, piece, side].wait_recv()
                if step == count - 1:
                    continue
                origin = member(spot - way * step)
                place = pl.ds(pl.multiple_of(origin * rows + offset, part), part)
                source = own_ref.at[pl.ds(offset, part)] if step == 0 else whole_ref.at[place]
                copies[step, piece, side] = send(
                    source, whole_ref.at[place], send_sem.at[step, piece, side],
                    recv_sem.at[step, piece, side], {"sp": targets[side]},
                )
        for side, way in enumerate(ways):
            if step:
                copies[step - 1, "slab", side].wait_recv()
            origin = member(spot - way * step)
            place = slab_place(origin, side)
            source = (
                slab_ref.at[pl.ds(side * half, half)]
                if step == 0
                else slabs_ref.at[group, place]
            )
            if step < count - 1:
                copies[step, "slab", side] = send(
                    source, slabs_ref.at[group, place], slab_send.at[step, side],
                    slab_recv.at[step, side], {"sp": targets[side]},
                )
            if step == 0:
                for number, peer in enumerate(peers if side == 0 else ()):
                    weights.append(
                        send(
                            stacked_ref, weight_ref.at[group], weight_send.at[number],
                            weight_recv.at[number], {"dp": peer},
                        )
                    )
            pass_on(step, side, source, place)
            start = origin * rows + side * PIECES * part
            backlog.append(pl.ds(pl.multiple_of(start, PIECES * part), PIECES * part))
        if step == 0:
            whole_ref[pl.ds(pl.multiple_of(me * rows, rows), rows), :] = own_ref[...]
            weight_ref[group] = stacked_ref[...]
            slabs_ref[group, pl.ds(pl.multiple_of(me * tall_slab, tall_slab), tall_slab), :] = (
                slab_ref[...]
            )
        if step == min(3, count - 1):
            for copy in weights:
                copy.wait_recv()
        if step >= min(3, count - 1):
            for place in backlog:
                project(place)
            backlog = []


    def remote(source, owner):
        return pltpu.make_async_remote_copy(
            src_ref=done_ref.at[owner], dst_ref=merged_ref.at[source],
            send_sem=done_send.at[owner], recv_sem=done_recv.at[source],
            device_id={"sp": owner}, device_id_type=MESH,
        )

    def one_block(index, unused):
        place = pl.ds(pl.multiple_of(index * block, block), block)
        projected = projected_ref[place, :]

        def unit(values, gain):
            values = values.astype(jnp.float32)
            scale = lax.rsqrt(jnp.mean(values * values, axis=-1, keepdims=True) + EPS)
            return values * scale * gain

        values_turned = projected[:, 2 * wide :].astype(jnp.float32).T
        lane = lax.broadcasted_iota(jnp.int32, (block, width), 1)
        ones_lanes = jnp.where(lane < 3, 1.0, 0.0)
        sub = lax.broadcasted_iota(jnp.int32, (2 * width, block), 0)
        ones_rows = jnp.where(
            lax.broadcasted_iota(jnp.int32, (16, block), 0) == 0, 1.0, 0.0
        )
        queries = []
        for head in range(heads):
            low = head * width
            query = unit(projected[:, low : low + width], gain_ref[0:1, :]) * width ** (-0.5)
            key = unit(projected[:, wide + low : wide + low + width], gain_ref[1:2, :])
            decay = -decay_ref[head : head + 1, place]
            first = decay.astype(jnp.bfloat16).astype(jnp.float32)
            rest = decay - first
            second = rest.astype(jnp.bfloat16).astype(jnp.float32)
            third = rest - second
            parts = jnp.where(
                sub == 0, first, jnp.where(sub == 1, second, jnp.where(sub == 2, third, 0.0))
            ).T
            queries.append(jnp.concatenate([query, ones_lanes], axis=1).astype(jnp.bfloat16))
            key_ref[head, place, :] = jnp.concatenate([key, parts[:, :width]], axis=1).astype(
                jnp.bfloat16
            )
            value_ref[head, index] = jnp.concatenate(
                [values_turned[low : low + width], ones_rows], axis=0
            ).astype(jnp.bfloat16)

        def step(column, carry, masked):
            fresh = []
            for head in range(heads):
                peak, total = carry[head]
                keys = key_ref[head, pl.ds(pl.multiple_of(column * block, block), block), :]
                scores = lax.dot_general(
                    keys, queries[head], DIMS_NT, preferred_element_type=jnp.float32
                )
                if masked:
                    key_place = lax.broadcasted_iota(jnp.int32, scores.shape, 0)
                    query_place = lax.broadcasted_iota(jnp.int32, scores.shape, 1)
                    scores = jnp.where(key_place <= query_place, scores, -jnp.inf)
                higher = jnp.maximum(peak, jnp.max(scores, axis=0, keepdims=True))
                probs = jnp.exp(scores - higher).astype(jnp.bfloat16)
                total = total * jnp.exp(peak - higher) + jnp.dot(
                    value_ref[head, column], probs, preferred_element_type=jnp.float32
                )
                fresh.append((higher, total))
            return tuple(fresh)

        start = tuple(
            (
                jnp.full((1, block), -1e30, jnp.float32),
                jnp.zeros((width + 16, block), jnp.float32),
            )
            for _ in range(heads)
        )
        carry = step(index, start, True)
        carry = lax.fori_loop(0, index, lambda column, c: step(column, c, False), carry)
        outs = []
        for head in range(heads):
            total = carry[head][1]
            mixed, norm = total[:width], total[width : width + 1]
            scale = lax.rsqrt(jnp.mean(mixed * mixed, axis=0, keepdims=True) + EPS * norm * norm)
            outs.append(mixed * scale)
        turned = jnp.concatenate(outs, axis=0).T.astype(jnp.bfloat16)
        for part_index in range(owners):
            owner = index * owners + part_index
            done_ref[owner] = turned[part_index * rows : (part_index + 1) * rows]

            @pl.when(owner != me)
            def _():
                remote(me, owner).start()

        return unused

    lax.fori_loop(0, count // owners, one_block, 0)
    merged_ref[me] = done_ref[me]
    for copy in passed:
        copy.wait_recv()
    for shift in range(1, count):
        other = lax.rem(me + shift, count)
        remote(other, other).wait_recv()
    merged = jnp.concatenate([merged_ref[source] for source in range(count)], axis=1)
    columns = slab_ref.shape[1]
    for place in range(groups):
        out_ref[:, place * columns : (place + 1) * columns] = jnp.dot(
            merged, slabs_ref[place], preferred_element_type=jnp.float32
        ).astype(out_ref.dtype)
    for copy in (*copies.values(), *passed, *weights):
        copy.wait_send()
    for shift in range(1, count):
        remote(me, lax.rem(me + shift, count)).wait_send()


def on_device(tokens, w_query, w_key, w_value, w_output, qk_gain, decay_sums):
    own_rows, decay_rows = tokens[0], decay_sums[0]
    count, groups = lax.axis_size("sp"), lax.axis_size("dp")
    rows, depth = own_rows.shape
    heads, width = decay_rows.shape[0], qk_gain.shape[1]
    wide, length, block = heads * width, count * rows, 2 * rows
    stacked = jnp.concatenate((w_query, w_key, w_value), axis=1)
    tall_slab, columns = w_output.shape
    bf16, sem = jnp.bfloat16, pltpu.SemaphoreType.DMA
    ring = (count - 1, PIECES, 2)
    result = pl.pallas_call(
        functools.partial(layer_kernel, heads, width, count, groups),
        out_shape=jax.ShapeDtypeStruct((rows, depth), bf16),
        in_specs=[pl.BlockSpec(memory_space=pltpu.VMEM)] * 5,
        out_specs=pl.BlockSpec(memory_space=pltpu.VMEM),
        scratch_shapes=[
            pltpu.VMEM((length, depth), bf16),
            pltpu.VMEM((groups, depth // groups, 3 * wide), bf16),
            pltpu.VMEM((groups, count * tall_slab, columns), bf16),
            pltpu.VMEM((length, 3 * wide), bf16),
            pltpu.VMEM((heads, length, 2 * width), bf16),
            pltpu.VMEM((heads, length // block, width + 16, block), bf16),
            pltpu.VMEM((count, rows, wide), bf16),
            pltpu.VMEM((count, rows, wide), bf16),
            sem(ring), sem(ring), sem((count - 1, 2)), sem((count - 1, 2)),
            sem((groups - 1, count, 2)), sem((groups - 1, count, 2)),
            sem((groups - 1,)), sem((groups - 1,)), sem((count,)), sem((count,)),
        ],
        compiler_params=pltpu.CompilerParams(
            collective_id=0, has_side_effects=True, vmem_limit_bytes=60 * 1024 * 1024
        ),
    )(own_rows, stacked, w_output, qk_gain, decay_rows)
    return result[None]


def solution(mesh):
    placed = (
        P("dp", "sp", None),
        P("dp", "sp"),
        P("dp", "sp"),
        P("dp", "sp"),
        P("sp", "dp"),
        P(),
        P("dp", "sp", None),
    )
    return jax.shard_map(
        on_device, mesh=mesh, in_specs=placed, out_specs=P("dp", "sp", None), check_vma=False
    )
```

```python
import functools

import jax
import jax.numpy as jnp
from jax import lax
from jax.experimental import pallas as pl
from jax.experimental.pallas import tpu as pltpu
from jax.sharding import PartitionSpec as P

EPS = 1e-06
DIMS_NT = (((1,), (1,)), ((), ()))


PIECES = 2
MESH = pl.DeviceIdType.MESH


def layer_kernel(
    heads, width, count, groups,
    own_ref, stacked_ref, slab_ref, gain_ref, decay_ref, out_ref,
    whole_ref, weight_ref, slabs_ref, projected_ref, key_ref, value_ref, done_ref, merged_ref,
    send_sem, recv_sem, slab_send, slab_recv, pass_send, pass_recv, weight_send, weight_recv,
    done_send, done_recv,
):
    rows, depth = own_ref.shape
    owners = 2
    block = owners * rows
    wide = heads * width
    part = rows // (2 * PIECES)
    tall = 4 if count % 4 == 0 else 1
    broad = count // tall
    me, group = lax.axis_index("sp"), lax.axis_index("dp")

    def member(spot):
        spot = lax.rem(spot + 2 * count, count)
        column, height = spot // tall, lax.rem(spot, tall)
        level = height + lax.rem(column, 2) * (tall - 1 - 2 * height)
        return level * broad + column

    level, column = me // broad, lax.rem(me, broad)
    spot = column * tall + level + lax.rem(column, 2) * (tall - 1 - 2 * level)
    ways = (1, -1)
    targets = [member(spot + way) for way in ways]
    peers = [lax.rem(group + shift, groups) for shift in range(1, groups)]

    barrier = pltpu.get_barrier_semaphore()
    for shift in range(1, count):
        other = lax.rem(me + shift, count)
        pl.semaphore_signal(barrier, inc=1, device_id={"sp": other}, device_id_type=MESH)
    for peer in peers:
        pl.semaphore_signal(barrier, inc=1, device_id={"dp": peer}, device_id_type=MESH)
    pl.semaphore_wait(barrier, count + groups - 2)

    def send(source, target, out_sem, in_sem, device):
        copy = pltpu.make_async_remote_copy(
            src_ref=source, dst_ref=target, send_sem=out_sem, recv_sem=in_sem,
            device_id=device, device_id_type=MESH,
        )
        copy.start()
        return copy

    tall_slab = slab_ref.shape[0]
    half = tall_slab // 2
    copies, passed, weights, backlog = {}, [], [], []

    def slab_place(origin, side):
        return pl.ds(pl.multiple_of(origin * tall_slab + side * half, half), half)

    def pass_on(step, side, source, place):
        for number, peer in enumerate(peers):
            passed.append(
                send(
                    source, slabs_ref.at[group, place], pass_send.at[number, step, side],
                    pass_recv.at[number, step, side], {"dp": peer},
                )
            )

    def project(place):
        projected_ref[place, :] = jnp.dot(
            whole_ref[place, :], weight_ref[...].reshape(depth, 3 * wide),
            preferred_element_type=jnp.float32,
        ).astype(jnp.bfloat16)

    for step in range(count):
        if step == min(2, count - 1):
            for copy in weights:
                copy.wait_recv()
        for piece in range(PIECES):
            for side, way in enumerate(ways):
                offset = (side * PIECES + piece) * part
                if step:
                    copies[step - 1, piece, side].wait_recv()
                if step == count - 1:
                    continue
                origin = member(spot - way * step)
                place = pl.ds(pl.multiple_of(origin * rows + offset, part), part)
                source = own_ref.at[pl.ds(offset, part)] if step == 0 else whole_ref.at[place]
                copies[step, piece, side] = send(
                    source, whole_ref.at[place], send_sem.at[step, piece, side],
                    recv_sem.at[step, piece, side], {"sp": targets[side]},
                )
            if 2 <= step < count - 1:
                for place in backlog[:2]:
                    project(place)
                backlog = backlog[2:]
        for side, way in enumerate(ways):
            if step:
                copies[step - 1, "slab", side].wait_recv()
            origin = member(spot - way * step)
            place = slab_place(origin, side)
            source = (
                slab_ref.at[pl.ds(side * half, half)]
                if step == 0
                else slabs_ref.at[group, place]
            )
            if step < count - 1:
                copies[step, "slab", side] = send(
                    source, slabs_ref.at[group, place], slab_send.at[step, side],
                    slab_recv.at[step, side], {"sp": targets[side]},
                )
            if step == 0:
                for number, peer in enumerate(peers if side == 0 else ()):
                    weights.append(
                        send(
                            stacked_ref, weight_ref.at[group], weight_send.at[number],
                            weight_recv.at[number], {"dp": peer},
                        )
                    )
            pass_on(step, side, source, place)
            start = origin * rows + side * PIECES * part
            backlog.append(pl.ds(pl.multiple_of(start, PIECES * part), PIECES * part))
        if step == 0:
            whole_ref[pl.ds(pl.multiple_of(me * rows, rows), rows), :] = own_ref[...]
            weight_ref[group] = stacked_ref[...]
            slabs_ref[group, pl.ds(pl.multiple_of(me * tall_slab, tall_slab), tall_slab), :] = (
                slab_ref[...]
            )
        if step == count - 1:
            for place in backlog:
                project(place)


    def remote(source, owner):
        return pltpu.make_async_remote_copy(
            src_ref=done_ref.at[owner], dst_ref=merged_ref.at[source],
            send_sem=done_send.at[owner], recv_sem=done_recv.at[source],
            device_id={"sp": owner}, device_id_type=MESH,
        )

    def one_block(index, unused):
        place = pl.ds(pl.multiple_of(index * block, block), block)
        projected = projected_ref[place, :]

        def unit(values, gain):
            values = values.astype(jnp.float32)
            scale = lax.rsqrt(jnp.mean(values * values, axis=-1, keepdims=True) + EPS)
            return values * scale * gain

        values_turned = projected[:, 2 * wide :].astype(jnp.float32).T
        lane = lax.broadcasted_iota(jnp.int32, (block, width), 1)
        ones_lanes = jnp.where(lane < 3, 1.0, 0.0)
        sub = lax.broadcasted_iota(jnp.int32, (2 * width, block), 0)
        ones_rows = jnp.where(
            lax.broadcasted_iota(jnp.int32, (16, block), 0) == 0, 1.0, 0.0
        )
        queries = []
        for head in range(heads):
            low = head * width
            query = unit(projected[:, low : low + width], gain_ref[0:1, :]) * width ** (-0.5)
            key = unit(projected[:, wide + low : wide + low + width], gain_ref[1:2, :])
            decay = -decay_ref[head : head + 1, place]
            first = decay.astype(jnp.bfloat16).astype(jnp.float32)
            rest = decay - first
            second = rest.astype(jnp.bfloat16).astype(jnp.float32)
            third = rest - second
            parts = jnp.where(
                sub == 0, first, jnp.where(sub == 1, second, jnp.where(sub == 2, third, 0.0))
            ).T
            queries.append(jnp.concatenate([query, ones_lanes], axis=1).astype(jnp.bfloat16))
            key_ref[head, place, :] = jnp.concatenate([key, parts[:, :width]], axis=1).astype(
                jnp.bfloat16
            )
            value_ref[head, index] = jnp.concatenate(
                [values_turned[low : low + width], ones_rows], axis=0
            ).astype(jnp.bfloat16)

        def step(column, carry, masked):
            fresh = []
            for head in range(heads):
                peak, total = carry[head]
                keys = key_ref[head, pl.ds(pl.multiple_of(column * block, block), block), :]
                scores = lax.dot_general(
                    keys, queries[head], DIMS_NT, preferred_element_type=jnp.float32
                )
                if masked:
                    key_place = lax.broadcasted_iota(jnp.int32, scores.shape, 0)
                    query_place = lax.broadcasted_iota(jnp.int32, scores.shape, 1)
                    scores = jnp.where(key_place <= query_place, scores, -jnp.inf)
                higher = jnp.maximum(peak, jnp.max(scores, axis=0, keepdims=True))
                probs = jnp.exp(scores - higher).astype(jnp.bfloat16)
                total = total * jnp.exp(peak - higher) + jnp.dot(
                    value_ref[head, column], probs, preferred_element_type=jnp.float32
                )
                fresh.append((higher, total))
            return tuple(fresh)

        start = tuple(
            (
                jnp.full((1, block), -1e30, jnp.float32),
                jnp.zeros((width + 16, block), jnp.float32),
            )
            for _ in range(heads)
        )
        carry = step(index, start, True)
        carry = lax.fori_loop(0, index, lambda column, c: step(column, c, False), carry)
        outs = []
        for head in range(heads):
            total = carry[head][1]
            mixed, norm = total[:width], total[width : width + 1]
            scale = lax.rsqrt(jnp.mean(mixed * mixed, axis=0, keepdims=True) + EPS * norm * norm)
            outs.append(mixed * scale)
        turned = jnp.concatenate(outs, axis=0).T.astype(jnp.bfloat16)
        for part_index in range(owners):
            owner = index * owners + part_index
            done_ref[owner] = turned[part_index * rows : (part_index + 1) * rows]

            @pl.when(owner != me)
            def _():
                remote(me, owner).start()

        return unused

    lax.fori_loop(0, count // owners, one_block, 0)
    merged_ref[me] = done_ref[me]
    for copy in passed:
        copy.wait_recv()
    for shift in range(1, count):
        other = lax.rem(me + shift, count)
        remote(other, other).wait_recv()
    merged = jnp.concatenate([merged_ref[source] for source in range(count)], axis=1)
    columns = slab_ref.shape[1]
    for place in range(groups):
        out_ref[:, place * columns : (place + 1) * columns] = jnp.dot(
            merged, slabs_ref[place], preferred_element_type=jnp.float32
        ).astype(out_ref.dtype)
    for copy in (*copies.values(), *passed, *weights):
        copy.wait_send()
    for shift in range(1, count):
        remote(me, lax.rem(me + shift, count)).wait_send()


def on_device(tokens, w_query, w_key, w_value, w_output, qk_gain, decay_sums):
    own_rows, decay_rows = tokens[0], decay_sums[0]
    count, groups = lax.axis_size("sp"), lax.axis_size("dp")
    rows, depth = own_rows.shape
    heads, width = decay_rows.shape[0], qk_gain.shape[1]
    wide, length, block = heads * width, count * rows, 2 * rows
    stacked = jnp.concatenate((w_query, w_key, w_value), axis=1)
    tall_slab, columns = w_output.shape
    bf16, sem = jnp.bfloat16, pltpu.SemaphoreType.DMA
    ring = (count - 1, PIECES, 2)
    result = pl.pallas_call(
        functools.partial(layer_kernel, heads, width, count, groups),
        out_shape=jax.ShapeDtypeStruct((rows, depth), bf16),
        in_specs=[pl.BlockSpec(memory_space=pltpu.VMEM)] * 5,
        out_specs=pl.BlockSpec(memory_space=pltpu.VMEM),
        scratch_shapes=[
            pltpu.VMEM((length, depth), bf16),
            pltpu.VMEM((groups, depth // groups, 3 * wide), bf16),
            pltpu.VMEM((groups, count * tall_slab, columns), bf16),
            pltpu.VMEM((length, 3 * wide), bf16),
            pltpu.VMEM((heads, length, 2 * width), bf16),
            pltpu.VMEM((heads, length // block, width + 16, block), bf16),
            pltpu.VMEM((count, rows, wide), bf16),
            pltpu.VMEM((count, rows, wide), bf16),
            sem(ring), sem(ring), sem((count - 1, 2)), sem((count - 1, 2)),
            sem((groups - 1, count, 2)), sem((groups - 1, count, 2)),
            sem((groups - 1,)), sem((groups - 1,)), sem((count,)), sem((count,)),
        ],
        compiler_params=pltpu.CompilerParams(
            collective_id=0, has_side_effects=True, vmem_limit_bytes=60 * 1024 * 1024
        ),
    )(own_rows, stacked, w_output, qk_gain, decay_rows)
    return result[None]


def solution(mesh):
    placed = (
        P("dp", "sp", None),
        P("dp", "sp"),
        P("dp", "sp"),
        P("dp", "sp"),
        P("sp", "dp"),
        P(),
        P("dp", "sp", None),
    )
    return jax.shard_map(
        on_device, mesh=mesh, in_specs=placed, out_specs=P("dp", "sp", None), check_vma=False
    )
```
